32 devices in a mesh: fs: 16 (over z, y, x), tp: 2 (over core).
Axes of the slice: x: 2, y: 2, z: 4, core: 2. Of those that a mesh axis runs over, the one named last changes fastest.
Arguments:
- tokens: bfloat16 [4096, 2048], P('fs'), may hold values from -6 to 6
- mix_gain: float32 [2048], replicated, may hold values from 0.1 to 1.9
- glu_value: bfloat16 [2048, 2048], P('fs', 'tp'), may hold values from -0.125 to 0.125
- glu_gate: bfloat16 [2048, 2048], P('fs', 'tp'), may hold values from -0.125 to 0.125
- conv_taps: float32 [31, 2048], P(None, 'tp'), may hold values from -2.2 to 2.2, as said below
- chan_gain: float32 [2048], P('tp'), may hold values from 0.1 to 1.9
- mix_out: bfloat16 [2048, 2048], P('tp', 'fs'), may hold values from -0.125 to 0.125
- mlp_gain: float32 [2048], replicated, may hold values from 0.1 to 1.9
- up_weight: bfloat16 [2048, 8192], P('fs', 'tp'), may hold values from -0.125 to 0.125
- down_weight: bfloat16 [8192, 2048], P('tp', 'fs'), may hold values from -0.0625 to 0.0625
Outputs:
- result: bfloat16 [4096, 2048], P('fs')
The draws below stay inside these ranges and needn't reach their ends.
Inputs may be any that keep to these rules, and one draw needn't show every extreme that they name: `conv_taps`: independent entries scaled by fan-in; channels fall into 16 groups of different scale.
All inputs are finite; a program needn't handle non-finite values.
Results may differ from the reference program's by a relative error of at most 0.018.
Values may be sent and summed in bfloat16 or wider, within the bound.
No kernel may reach another device: no remote copies, remote signals or barrier semaphores. Data moves between devices by JAX's collectives and lax.ppermute only.
A program may use at most 128 MiB of HBM per device.

```python
import jax
import jax.numpy as jnp
from jax import lax

D = 2048
C = 2048
FF = 8192
WIDTH = 31
LEN = 128
TOKENS = 4096
N_TP = 2


def draw_conv_taps(key, part):
    first, second = jax.random.split(key)
    raw_taps = jnp.clip(jax.random.normal(first, (WIDTH, C), jnp.float32), -4.0, 4.0)
    levels = jnp.exp(jax.random.uniform(second, (16,), jnp.float32, jnp.log(0.3), jnp.log(3.0)))
    return raw_taps * WIDTH ** (-0.5) * jnp.repeat(levels, C // 16)


def block_scale(own_key, dims, shards, smallest, largest):
    def one(position, shards_of):
        heights = jax.random.uniform(jax.random.fold_in(jax.random.fold_in(own_key, 6), position), (shards_of,), jnp.float32, smallest / len(shards), largest / len(shards))
        return jnp.repeat(jnp.exp(heights), dims[position] // shards_of).reshape((-1,) + (1,) * (len(dims) - position - 1))

    level = one(*shards[0])
    for cut in shards[1:]:
        level = level * one(*cut)
    return level


def centred(stream_key, dims, scale, limit, shards=(), held_as=jnp.bfloat16):
    values = jax.random.normal(stream_key, dims, jnp.float32) * scale
    if len(shards) > 0:
        values = block_scale(stream_key, dims, shards, -0.22, 0.18) * values
    return jnp.clip(values, min=-limit, max=limit).astype(held_as)


def setup_inputs(seed: int = 0) -> dict:
    streams_of = jax.random.split(jax.random.key(seed), 11)
    tokens = centred(streams_of[0], (TOKENS, D), 1.0, 6.0, ((0, 16),))
    mix_gain = jnp.clip(1.0 + 0.18 * jax.random.normal(streams_of[1], (D,), jnp.float32), 0.1, 1.9)
    glu_value = centred(streams_of[2], (D, C), D ** -0.5, 0.125, ((0, 16), (1, 2)))
    glu_gate = centred(streams_of[3], (D, C), D ** -0.5, 0.125, ((0, 16), (1, 2)))
    conv_taps = draw_conv_taps(jax.random.fold_in(streams_of[10], 71), 0)
    chan_gain = jnp.clip(1.0 + 0.18 * jax.random.normal(streams_of[5], (C,), jnp.float32), 0.1, 1.9)
    mix_out = centred(streams_of[6], (C, D), C ** -0.5, 0.125, ((0, 2), (1, 16)))
    mlp_gain = jnp.clip(1.0 + 0.18 * jax.random.normal(streams_of[7], (D,), jnp.float32), 0.1, 1.9)
    up_weight = centred(streams_of[8], (D, FF), D ** -0.5, 0.125, ((0, 16), (1, 2)))
    down_weight = centred(streams_of[9], (FF, D), FF ** -0.5, 0.0625, ((0, 2), (1, 16)))
    return {"tokens": tokens, "mix_gain": mix_gain, "glu_value": glu_value, "glu_gate": glu_gate, "conv_taps": conv_taps, "chan_gain": chan_gain, "mix_out": mix_out, "mlp_gain": mlp_gain, "up_weight": up_weight, "down_weight": down_weight}


norm_floor = 0.05

def rms_scale(stream, gain):
    return stream * lax.rsqrt(lax.optimization_barrier(jnp.mean(stream * stream, axis=-1, keepdims=True)) + norm_floor) * gain

def bf16_round(value):
    return lax.optimization_barrier(value.astype(jnp.bfloat16)).astype(jnp.float32)

def depthwise(glu, conv_taps):
    seqs = glu.shape[0] // LEN
    blocks = glu.reshape(seqs, LEN, glu.shape[1]).astype(jnp.float32)
    reach = conv_taps.shape[0] // 2
    padded = jnp.pad(blocks, ((0, 0), (reach, reach), (0, 0)))
    total = jnp.zeros_like(blocks)
    for offset in range(conv_taps.shape[0]):
        total = total + padded[:, offset:offset + LEN] * conv_taps[offset]
    return total.reshape(glu.shape)

def shard_sum(left, right):
    block = left.shape[1] // N_TP
    total = jnp.zeros((left.shape[0], right.shape[1]), jnp.float32)
    for shard in range(N_TP):
        partial_term = jnp.dot(left[:, shard * block:(shard + 1) * block], right[shard * block:(shard + 1) * block], preferred_element_type=jnp.float32)
        total = total + bf16_round(partial_term)
    return total.astype(jnp.bfloat16)

def reference(tokens, mix_gain, glu_value, glu_gate, conv_taps, chan_gain, mix_out, mlp_gain, up_weight, down_weight):
    stream = tokens.astype(jnp.float32)
    normed = rms_scale(stream, mix_gain).astype(jnp.bfloat16)
    values = jnp.dot(normed, glu_value, preferred_element_type=jnp.float32)
    gating = jnp.dot(normed, glu_gate, preferred_element_type=jnp.float32)
    glu = (values * jax.nn.sigmoid(gating)).astype(jnp.bfloat16)
    convolved = depthwise(glu, conv_taps)
    centre = lax.optimization_barrier(jnp.mean(convolved, axis=-1, keepdims=True))
    spread = lax.optimization_barrier(jnp.mean(convolved * convolved, axis=-1, keepdims=True)) - centre * centre
    hidden = jax.nn.silu((convolved - centre) * lax.rsqrt(spread + norm_floor) * chan_gain).astype(jnp.bfloat16)
    mixed = shard_sum(hidden, mix_out)
    resid = stream + mixed.astype(jnp.float32)
    normed_mlp = rms_scale(resid, mlp_gain).astype(jnp.bfloat16)
    active = jnp.square(jax.nn.relu(jnp.dot(normed_mlp, up_weight, preferred_element_type=jnp.float32))).astype(jnp.bfloat16)
    feed = shard_sum(active, down_weight)
    return (resid + feed.astype(jnp.float32)).astype(jnp.bfloat16)
```

```python
import math

import jax
import jax.numpy as jnp
from jax import lax
from jax.sharding import PartitionSpec as P

LEN = 128
norm_floor = 0.05


def rms_scale(stream, gain):
    return stream * lax.rsqrt(jnp.mean(stream * stream, axis=-1, keepdims=True) + norm_floor) * gain


def bf16_round(value):
    return lax.optimization_barrier(value.astype(jnp.bfloat16)).astype(jnp.float32)


def depthwise(glu, taps):
    s, tokens, c = glu.shape
    blocks = glu.reshape(s, tokens // LEN, LEN, c).astype(jnp.float32)
    reach = taps.shape[0] // 2
    padded = jnp.pad(blocks, ((0, 0), (0, 0), (reach, reach), (0, 0)))
    total = jnp.zeros_like(blocks)
    for offset in range(taps.shape[0]):
        total = total + padded[:, :, offset : offset + LEN] * taps[offset][:, None, None]
    return total.reshape(glu.shape)


class Plan:
    def __init__(self, mesh, rows):
        self.fs, self.tp = mesh.shape["fs"], mesh.shape["tp"]
        self.plane = math.gcd(self.fs, 4)
        self.lines = self.fs // self.plane
        self.split = math.gcd(self.tp, rows // LEN)
        self.other = self.tp // self.split
        m, k, s, h = self.plane, self.lines, self.split, self.other
        self.plane_groups = [[z * m + q for q in range(m)] for z in range(k)]
        self.line_groups = [
            [(z * m + q) * self.tp + o * s + j for j in range(s) for z in range(k)]
            for q in range(m)
            for o in range(h)
        ]
        self.token_groups = [
            [(z * m + q) * self.tp + o * s + j for q in range(m) for o in range(h)]
            for z in range(k)
            for j in range(s)
        ]
        self.split_groups = [[o * s + j for j in range(s)] for o in range(h)]
        self.other_groups = [[o * s + j for o in range(h)] for j in range(s)]

    def exchange(self, x):
        return lax.all_to_all(
            x, "fs", axis_index_groups=self.plane_groups, split_axis=0, concat_axis=0, tiled=True
        )

    def weight(self, x):
        x = self.exchange(x).reshape(-1, x.shape[-1])
        x = lax.all_gather(
            x, ("fs", "tp"), axis_index_groups=self.line_groups, axis=0, tiled=True
        )
        return x.reshape(self.split, -1, x.shape[-1])

    def share(self, x):
        wide = jnp.broadcast_to(x[None], (self.plane,) + x.shape)
        return self.exchange(wide).reshape(-1, x.shape[-1])

    def reduce(self, x):
        x = self.exchange(x.reshape(self.plane, -1, x.shape[-1])).astype(jnp.float32)
        total = jnp.sum(x, axis=0)
        if self.other > 1:
            total = lax.psum(total, "tp", axis_index_groups=self.other_groups)
        return total


def columns(x, parts):
    return jnp.transpose(x.reshape(x.shape[0], parts, -1), (1, 0, 2))


def rows_t(x, parts):
    return jnp.transpose(x.reshape(parts, -1, x.shape[1]), (0, 2, 1))


def build(plan):
    def per_device(
        tokens,
        mix_gain,
        glu_value,
        glu_gate,
        conv_taps,
        chan_gain,
        mix_out,
        mlp_gain,
        up_weight,
        down_weight,
    ):
        m, s = plan.plane, plan.split
        place = lax.axis_index("tp") % s
        member = lax.axis_index("fs") % m
        own = tokens.shape[0] // s
        stream = lax.dynamic_slice_in_dim(tokens, place * own, own, 0).astype(jnp.float32)
        channels = glu_value.shape[1] * plan.tp

        w_glu = plan.weight(
            jnp.concatenate([columns(glu_value, m), columns(glu_gate, m)], axis=2)
        )
        w_mix = plan.weight(rows_t(mix_out, m))
        w_up = plan.weight(columns(up_weight, m))
        w_down = plan.weight(rows_t(down_weight, m))
        cq = w_mix.shape[2]

        small = jnp.concatenate([conv_taps, chan_gain[None]], axis=0)
        small = lax.dynamic_slice_in_dim(small, member * cq, cq, 1)
        small = lax.all_gather(small, "tp", axis_index_groups=plan.split_groups, axis=1)
        taps, gain = small[:-1], small[-1]

        normed = plan.share(rms_scale(stream, mix_gain).astype(jnp.bfloat16))
        both = jnp.einsum("td,sdn->stn", normed, w_glu, preferred_element_type=jnp.float32)
        glu = (both[..., :cq] * jax.nn.sigmoid(both[..., cq:])).astype(jnp.bfloat16)
        convolved = depthwise(glu, taps)
        sums, squares = lax.psum(
            (jnp.sum(convolved, axis=(0, 2)), jnp.sum(convolved * convolved, axis=(0, 2))),
            ("fs", "tp"),
            axis_index_groups=plan.token_groups,
        )
        centre = (sums / channels)[:, None]
        spread = (squares / channels)[:, None] - centre * centre
        hidden = jax.nn.silu(
            (convolved - centre) * lax.rsqrt(spread + norm_floor) * gain[:, None]
        ).astype(jnp.bfloat16)
        mixed = plan.reduce(
            jnp.einsum("stc,sdc->td", hidden, w_mix, preferred_element_type=jnp.float32).astype(
                jnp.bfloat16
            )
        )
        resid = stream + bf16_round(mixed)
        normed_mlp = plan.share(rms_scale(resid, mlp_gain).astype(jnp.bfloat16))
        active = jnp.square(
            jax.nn.relu(
                jnp.einsum("td,sdf->stf", normed_mlp, w_up, preferred_element_type=jnp.float32)
            )
        ).astype(jnp.bfloat16)
        feed = plan.reduce(
            jnp.einsum("stf,sdf->td", active, w_down, preferred_element_type=jnp.float32).astype(
                jnp.bfloat16
            )
        )
        finished = (resid + bf16_round(feed)).astype(jnp.bfloat16)
        whole = jnp.zeros((s,) + finished.shape, finished.dtype)
        whole = lax.dynamic_update_slice_in_dim(whole, finished[None], place, 0)
        for step in range(1, s):
            pairs = [
                (group[j], group[(j + step) % s]) for group in plan.split_groups for j in range(s)
            ]
            piece = lax.ppermute(finished, "tp", pairs)
            whole = lax.dynamic_update_slice_in_dim(whole, piece[None], (place - step) % s, 0)
        return whole.reshape(tokens.shape)

    return per_device


def solution(mesh):
    in_specs = (
        P("fs", None),
        P(),
        P("fs", "tp"),
        P("fs", "tp"),
        P(None, "tp"),
        P("tp"),
        P("tp", "fs"),
        P(),
        P("fs", "tp"),
        P("tp", "fs"),
    )
    out_specs = P("fs", None)

    def step(tokens, *rest):
        plan = Plan(mesh, tokens.shape[0] // mesh.shape["fs"])
        return jax.shard_map(
            build(plan), mesh=mesh, in_specs=in_specs, out_specs=out_specs, check_vma=False
        )(tokens, *rest)

    return step
```
